32 devices in a mesh: sp: 4 (over z), dp: 8 (over y, x, core).
Axes of the slice: x: 2, y: 2, z: 4, core: 2. Of those that a mesh axis runs over, the one named last changes fastest.
Arguments:
- inputs: bfloat16 [8, 512, 2048], P('dp', 'sp'), may hold values from -6 to 6
- queries: bfloat16 [8, 512, 1024], P('dp', 'sp'), may hold values from -6 to 6
- keys: bfloat16 [8, 512, 1024], P('dp', 'sp'), may hold values from -1.5 to 1.5
- values: bfloat16 [8, 512, 1024], P('dp', 'sp'), may hold values from -6 to 6
- log_decay: bfloat16 [8, 512, 1024], P('dp', 'sp'), may hold values from -0.1 to 0, as said below
- cotangent: bfloat16 [8, 512, 1024], P('dp', 'sp'), may hold values from -0.59765625 to 0.59765625
- value_weight: bfloat16 [2048, 1024], P('dp'), may hold values from -0.125 to 0.125
Outputs:
- grad_queries: bfloat16 [8, 512, 1024], P('dp', 'sp')
- grad_keys: bfloat16 [8, 512, 1024], P('dp', 'sp')
- grad_decay: bfloat16 [8, 512, 1024], P('dp', 'sp')
- grad_inputs: bfloat16 [8, 512, 2048], P('dp', 'sp')
- grad_weight: float32 [2048, 1024], P('dp')
The draws below stay inside these ranges and needn't reach their ends.
Inputs may be any that keep to these rules, and one draw needn't show every extreme that they name: `log_decay`: the log decays are negative; per key channel and sequence they differ between positions.
All inputs are finite; a program needn't handle non-finite values.
Results may differ from the reference program's by a relative error of at most 0.015.
Values may be sent and summed in bfloat16 or wider, within the bound.
A program may use at most 128 MiB of HBM per device.

```python
import math
import jax
import jax.numpy as jnp
from jax import lax

D = 2048
HEADS = 16
HEAD_DIM = 64
BLOCK = 128
HALF = 32
GROUPS = 32
WIDTH = 1024
SEQ = 512
SEQS = 8


def draw_log_decay(key, part):
    keys_list = jax.random.split(key, 5)
    share = 0.5
    slow_pick = jax.random.uniform(keys_list[0], (SEQS, 1, WIDTH), jnp.float32) < share
    fast_rate = jax.random.uniform(keys_list[1], (SEQS, 1, WIDTH), jnp.float32, 1.0 / 50.0, 1.0 / 30.0)
    slow_rate = jax.random.uniform(keys_list[2], (SEQS, 1, WIDTH), jnp.float32, 0.2, 0.5) / SEQ
    base_rate = jnp.where(slow_pick, slow_rate, fast_rate)
    block_count = SEQ // BLOCK
    block_factor = jnp.exp(jax.random.uniform(keys_list[3], (SEQS, block_count, 1, WIDTH), jnp.float32, -math.log(2.0), math.log(2.0)))
    block_factor = jnp.broadcast_to(block_factor, (SEQS, block_count, BLOCK, WIDTH)).reshape(SEQS, SEQ, WIDTH)
    token_factor = jnp.exp(jax.random.uniform(keys_list[4], (SEQS, SEQ, WIDTH), jnp.float32, math.log(0.7), math.log(1.4)))
    return (-(base_rate * block_factor * token_factor)).astype(jnp.bfloat16)


def levels(stream_key, extent, cuts, low, high):
    gain = 1.0
    for axis_at, parts in cuts:
        steps = jax.random.uniform(jax.random.fold_in(jax.random.fold_in(stream_key, 6), axis_at), (parts,), jnp.float32, low / len(cuts), high / len(cuts))
        gain = gain * jnp.repeat(jnp.exp(steps), extent[axis_at] // parts).reshape((-1,) + (1,) * (len(extent) - 1 - axis_at))
    return gain


def scatter_about(rng, shape, scale, limit, cuts=(), dtype=jnp.bfloat16):
    result = jax.random.normal(rng, shape, jnp.float32) * scale
    if len(cuts) > 0:
        result = levels(rng, shape, cuts, -0.22, 0.18) * result
    return jnp.clip(result, min=-limit, max=limit).astype(dtype)


def setup_inputs(seed: int = 0) -> dict:
    key_of = jax.random.split(jax.random.key(seed), 8)
    inputs = scatter_about(key_of[0], (SEQS, SEQ, D), 1.0, 6.0, ((0, 8), (1, 4)))
    queries = scatter_about(key_of[1], (SEQS, SEQ, WIDTH), 1.0, 6.0, ((0, 8), (1, 4)))
    keys = scatter_about(key_of[2], (SEQS, SEQ, WIDTH), 0.25, 1.5, ((0, 8), (1, 4)))
    values = scatter_about(key_of[3], (SEQS, SEQ, WIDTH), 1.0, 6.0, ((0, 8), (1, 4)))
    log_decay = draw_log_decay(jax.random.fold_in(key_of[7], 71), 0)
    cotangent = scatter_about(key_of[5], (SEQS, SEQ, WIDTH), 0.1, 0.59765625, ((0, 8), (1, 4)))
    value_weight = scatter_about(key_of[6], (D, WIDTH), D ** -0.5, 0.125, ((0, 8),))
    return {"inputs": inputs, "queries": queries, "keys": keys, "values": values, "log_decay": log_decay, "cotangent": cotangent, "value_weight": value_weight}


def combine(earlier, later):
    first_decay, first_state = earlier
    second_decay, second_state = later
    return (first_decay * second_decay, second_decay[..., None] * first_state + second_state)

def carry_scan(decays, updates):
    return lax.associative_scan(combine, (decays, updates), axis=0)[1]

def to_blocks(rows, num_blocks):
    length, groups, width = rows.shape
    return jnp.transpose(rows.astype(jnp.float32).reshape(num_blocks, BLOCK, groups, width), (0, 2, 3, 1))

def mixing(query_rows, key_rows, value_rows, gate_rows):
    length, groups, key_width = query_rows.shape
    value_width = value_rows.shape[2]
    num_blocks = length // BLOCK
    scaled_query = to_blocks(query_rows, num_blocks) * HEAD_DIM ** (-0.5)
    key_float = to_blocks(key_rows, num_blocks)
    value_float = to_blocks(value_rows, num_blocks)
    gate_float = to_blocks(gate_rows, num_blocks)
    running = jnp.cumsum(gate_float, axis=3)
    exclusive = running - gate_float
    block_end = running[..., -1]
    lower_mask = jnp.tril(jnp.ones((BLOCK, BLOCK), jnp.float32))
    upper_mask = lower_mask.T
    query_fwd = scaled_query * jnp.exp(running)
    key_fwd = key_float * jnp.exp(-running)
    scores_fwd = jnp.einsum('ngcr,ngcs->ngrs', query_fwd, key_fwd) * lower_mask
    key_end = key_float * jnp.exp(block_end[..., None] - running)
    states = carry_scan(jnp.exp(block_end), jnp.einsum('ngcs,ngvs->ngcv', key_end, value_float))
    before = jnp.concatenate([jnp.zeros_like(states[:1]), states[:-1]], axis=0)
    out_fwd = jnp.einsum('ngrs,ngvs->ngvr', scores_fwd, value_float) + jnp.einsum('ngcr,ngcv->ngvr', query_fwd, before)
    query_bwd = scaled_query * jnp.exp(-exclusive)
    key_bwd = key_float * jnp.exp(exclusive)
    scores_bwd = jnp.einsum('ngcr,ngcs->ngrs', query_bwd, key_bwd) * upper_mask
    rights = jnp.flip(carry_scan(jnp.flip(jnp.exp(block_end), 0), jnp.flip(jnp.einsum('ngcs,ngvs->ngcv', key_bwd, value_float), 0)), 0)
    after = jnp.concatenate([rights[1:], jnp.zeros_like(rights[:1])], axis=0)
    query_read = scaled_query * jnp.exp(block_end[..., None] - exclusive)
    out_bwd = jnp.einsum('ngrs,ngvs->ngvr', scores_bwd, value_float) + jnp.einsum('ngcr,ngcv->ngvr', query_read, after)
    total = out_fwd + out_bwd
    return jnp.transpose(total, (0, 3, 1, 2)).reshape(length, groups, value_width)

def reference(inputs, queries, keys, values, log_decay, cotangent, value_weight):
    seq_len = queries.shape[1]
    width = queries.shape[2]

    def per_group(array):
        spread = jnp.broadcast_to(array.reshape(seq_len, HEADS, 1, HEAD_DIM), (seq_len, HEADS, 2, HEAD_DIM))
        return spread.reshape(seq_len, GROUPS, HEAD_DIM)

    def one_sequence(pieces):
        query_seq, key_seq, value_seq, gate_seq, upstream = pieces
        _, pullback = jax.vjp(mixing, query_seq.reshape(seq_len, GROUPS, HALF), key_seq.reshape(seq_len, GROUPS, HALF), per_group(value_seq), gate_seq.reshape(seq_len, GROUPS, HALF))
        grad_q, grad_k, grad_v, grad_g = pullback(per_group(upstream).astype(jnp.float32))
        value_sum = lax.optimization_barrier(jnp.sum(grad_v.astype(jnp.bfloat16).astype(jnp.float32).reshape(seq_len, HEADS, 2, HEAD_DIM), axis=2))
        return (grad_q.astype(jnp.bfloat16).reshape(seq_len, width), grad_k.astype(jnp.bfloat16).reshape(seq_len, width), grad_g.astype(jnp.bfloat16).reshape(seq_len, width), value_sum.astype(jnp.bfloat16).reshape(seq_len, width))
    grad_queries, grad_keys, grad_decay, value_grad = lax.map(one_sequence, (queries, keys, values, log_decay, cotangent))
    flat_inputs = inputs.reshape(-1, inputs.shape[2])
    flat_grad = value_grad.reshape(-1, width)
    grad_inputs = jnp.dot(flat_grad, value_weight.T, preferred_element_type=jnp.float32).astype(jnp.bfloat16).reshape(inputs.shape)
    grad_weight = jnp.dot(flat_inputs.T, flat_grad, preferred_element_type=jnp.float32)
    return (grad_queries, grad_keys, grad_decay, grad_inputs, grad_weight)
```

```python
import functools

import jax
import jax.numpy as jnp
from jax import lax
from jax.experimental import pallas as pl
from jax.experimental.pallas import tpu as pltpu
from jax.sharding import PartitionSpec as P

HEAD_DIM = 64
PAIR = 128
BF = jnp.bfloat16
F32 = jnp.float32


def nt(a, b):
    return lax.dot_general(a, b, (((1,), (1,)), ((), ())), preferred_element_type=F32)


def nn(a, b):
    return lax.dot_general(a, b, (((1,), (0,)), ((), ())), preferred_element_type=F32)


def tn(a, b):
    return lax.dot_general(a, b, (((0,), (0,)), ((), ())), preferred_element_type=F32)


def split(a):
    hi = a.astype(BF)
    return hi, (a - hi.astype(F32)).astype(BF)


def kernel(
    sp, chips, chunks,
    x_ref, q_ref, k_ref, v_ref, g_ref, o_ref, w_ref,
    dq_ref, dk_ref, dg_ref, gi_ref, gw_ref,
    qf_s, kf_s, qb_s, kb_s, ke_s, qr_s,
    ec_s, en_s, ex_s, enx_s, eer_s,
    dqf_s, dqb_s, dkf_s, dkb_s, dv_s,
    sf_s, sb_s, ee_s,
    fin, bin_, fout, bout,
    xin, xt, vgs, wpair, gin, gout,
    half_out, half_in, part, gfin, gbin, gfout, gbout,
    s_f, r_f, s_b, r_b, s_x, r_x, s_v, r_v, s_w, r_w, s_g, r_g, s_h, r_h,
    s_gf, r_gf, s_gb, r_gb, loc,
):
    tokens, width = q_ref.shape
    pairs = width // PAIR
    rows = w_ref.shape[0]
    z = lax.axis_index("sp")
    d = lax.axis_index("dp")
    chip = d // 2
    core = lax.rem(d, 2)
    partner = chip * 2 + (1 - core)
    first = z == 0
    last = z == sp - 1
    inner = jnp.logical_and(z > 0, z < sp - 1)
    lower_half = z < sp // 2

    def peer(j):
        other = lax.rem(chip + j, chips)
        return other, other * 2 + core

    barrier = pltpu.get_barrier_semaphore()
    for j in range(1, chips):
        pl.semaphore_signal(barrier, inc=1, device_id={"dp": peer(j)[1]})
    pl.semaphore_signal(barrier, inc=1, device_id={"dp": partner})

    for step in (1, sp - 1):
        pl.semaphore_signal(barrier, inc=1, device_id={"sp": lax.rem(z + step, sp)})
    pl.semaphore_wait(barrier, chips + 2)

    def mine(i):
        return pl.ds(pl.multiple_of(i * tokens, tokens), tokens)

    def chip_cols(i):
        return pl.ds(pl.multiple_of(i * 2 * rows, 2 * rows), 2 * rows)

    def copy_x(j):
        other, idx = peer(j)
        return pltpu.make_async_remote_copy(
            x_ref.at[:, chip_cols(other)], xin.at[mine(chip)], s_x.at[j], r_x.at[j],
            device_id={"dp": idx})

    def copy_w():
        return pltpu.make_async_remote_copy(
            w_ref, wpair.at[pl.ds(pl.multiple_of(core * rows, rows), rows)], s_w, r_w,
            device_id={"dp": partner})

    def lanes(p):
        return pl.ds(pl.multiple_of(p * PAIR, PAIR), PAIR)

    def copy_v(j, p):
        _, idx = peer(j)
        return pltpu.make_async_remote_copy(
            vgs.at[mine(chip), lanes(p)], vgs.at[mine(chip), lanes(p)],
            s_v.at[j, p], r_v.at[j, p], device_id={"dp": idx})

    def copy_f(p):
        return pltpu.make_async_remote_copy(
            fout.at[p], fin.at[p], s_f.at[p], r_f.at[p], device_id={"sp": z + 1})

    def copy_b(p):
        return pltpu.make_async_remote_copy(
            bout.at[p], bin_.at[p], s_b.at[p], r_b.at[p], device_id={"sp": z - 1})

    for j in range(1, chips):
        copy_x(j).start()
    copy_w().start()
    own_x = pltpu.make_async_copy(x_ref.at[:, chip_cols(chip)], xin.at[mine(chip)], loc.at[0])
    own_x.start()
    own_w = pltpu.make_async_copy(
        w_ref, wpair.at[pl.ds(pl.multiple_of(core * rows, rows), rows)], loc.at[1])
    own_w.start()

    @pl.when(first)
    def _():
        fin[...] = jnp.zeros_like(fin)

    @pl.when(last)
    def _():
        bin_[...] = jnp.zeros_like(bin_)

    ti = lax.broadcasted_iota(jnp.int32, (tokens, tokens), 0)
    tj = lax.broadcasted_iota(jnp.int32, (tokens, tokens), 1)
    tril = jnp.where(tj <= ti, 1.0, 0.0).astype(BF)
    triu = jnp.where(tj >= ti, 1.0, 0.0).astype(BF)
    ci = lax.broadcasted_iota(jnp.int32, (PAIR, PAIR), 0)
    cj = lax.broadcasted_iota(jnp.int32, (PAIR, PAIR), 1)
    diag = (ci < HEAD_DIM) == (cj < HEAD_DIM)
    ones_c = jnp.ones((tokens, PAIR), BF)
    left = lax.broadcasted_iota(jnp.int32, (tokens, PAIR), 1) < HEAD_DIM
    ri = lax.broadcasted_iota(jnp.int32, (2 * tokens, tokens), 0)
    rj = lax.broadcasted_iota(jnp.int32, (2 * tokens, tokens), 1)
    rt = jnp.where(ri >= tokens, ri - tokens, ri)
    low2 = rt >= rj
    up2 = rt <= rj

    def stack(a):
        zero = jnp.zeros_like(a)
        return jnp.concatenate([jnp.where(left, a, zero), jnp.where(left, zero, a)], axis=0)

    def phase_a(p, carry):
        sl = lanes(p)
        gate = g_ref[:, sl]
        run = nn(tril, gate)
        excl = run - gate.astype(F32)
        ec = jnp.exp(run)
        en = jnp.exp(-run)
        ex = jnp.exp(excl)
        enx = jnp.exp(-excl)
        eer = ec[tokens - 1:tokens, :]
        qs = q_ref[:, sl].astype(F32) * HEAD_DIM ** (-0.5)
        ks = k_ref[:, sl].astype(F32)
        qf = (qs * ec).astype(BF)
        kb = (ks * ex).astype(BF)
        ke = (ks * (en * eer)).astype(BF)
        qr = (qs * (enx * eer)).astype(BF)
        qf_s[:, sl] = qf
        kf_s[:, sl] = (ks * en).astype(BF)
        qb_s[:, sl] = (qs * enx).astype(BF)
        kb_s[:, sl] = kb
        ke_s[:, sl] = ke
        qr_s[:, sl] = qr
        ec_s[:, sl] = ec
        en_s[:, sl] = en
        ex_s[:, sl] = ex
        enx_s[:, sl] = enx
        eer_s[:, sl] = jnp.broadcast_to(eer, (8, PAIR))
        val = v_ref[:, sl]
        cot = o_ref[:, sl]
        cot_r = pltpu.roll(cot.astype(F32), HEAD_DIM, 1).astype(BF)
        sf = jnp.where(diag, tn(ke, val), tn(qr, cot_r))
        sb = jnp.where(diag, tn(kb, val), tn(qf, cot_r))
        sf_s[p] = sf
        sb_s[p] = sb
        ee_s[p] = jnp.exp(tn(gate, ones_c))

        @pl.when(first)
        def _():
            fout[p] = sf.astype(BF)
            copy_f(p).start()

        @pl.when(last)
        def _():
            bout[p] = sb.astype(BF)
            copy_b(p).start()

        return carry

    lax.fori_loop(0, pairs, phase_a, 0)

    def forward_step(p):
        copy_f(p).wait_recv()

        @pl.when(z < sp - 1)
        def _():
            fout[p] = (ee_s[p] * fin[p].astype(F32) + sf_s[p]).astype(BF)
            copy_f(p).start()

    def backward_step(p):
        copy_b(p).wait_recv()

        @pl.when(z > 0)
        def _():
            bout[p] = (ee_s[p] * bin_[p].astype(F32) + sb_s[p]).astype(BF)
            copy_b(p).start()

    def phase_b(p, carry):
        sl = lanes(p)
        qf2 = stack(qf_s[:, sl])
        qb2 = stack(qb_s[:, sl])
        cot2 = stack(o_ref[:, sl])
        kf = kf_s[:, sl]
        kb = kb_s[:, sl]
        score = jnp.where(low2, nt(qf2, kf), 0.0) + jnp.where(up2, nt(qb2, kb), 0.0)
        dscore = nt(cot2, v_ref[:, sl])
        dlow = jnp.where(low2, dscore, 0.0).astype(BF)
        dup = jnp.where(up2, dscore, 0.0).astype(BF)
        dv_s[:, sl] = tn(score.astype(BF), cot2)
        dkf_s[:, sl] = tn(dlow, qf2)
        dkb_s[:, sl] = tn(dup, qb2)
        dqf_s[:, sl] = nn(jnp.concatenate([dlow[:tokens], dlow[tokens:]], axis=1), stack(kf))
        dqb_s[:, sl] = nn(jnp.concatenate([dup[:tokens], dup[tokens:]], axis=1), stack(kb))

        @pl.when(jnp.logical_and(lower_half, z > 0))
        def _():
            forward_step(p)

        @pl.when(jnp.logical_and(jnp.logical_not(lower_half), z < sp - 1))
        def _():
            backward_step(p)

        return carry

    lax.fori_loop(0, pairs, phase_b, 0)

    def phase_c(p, carry):
        sl = lanes(p)

        @pl.when(jnp.logical_and(lower_half, z < sp - 1))
        def _():
            backward_step(p)

        @pl.when(jnp.logical_and(jnp.logical_not(lower_half), z > 0))
        def _():
            forward_step(p)

        f_in = fin[p].astype(F32)
        b_in = bin_[p].astype(F32)
        b_roll = pltpu.roll(b_in, HEAD_DIM, 1)
        before = jnp.where(diag, f_in, 0.0).astype(BF)
        gb = jnp.where(diag, pltpu.roll(f_in, HEAD_DIM, 1), 0.0).astype(BF)
        after = jnp.where(diag, b_in, 0.0).astype(BF)
        gf = jnp.where(diag, b_roll, 0.0).astype(BF)
        val = v_ref[:, sl]
        cot = o_ref[:, sl]
        ke = ke_s[:, sl]
        kb = kb_s[:, sl]
        dv = dv_s[:, sl] + nn(ke, gf) + nn(kb, gb)
        vgs[mine(chip), sl] = dv.astype(BF)
        for j in range(1, chips):
            copy_v(j, p).start()
        dqf = dqf_s[:, sl] + nt(cot, before)
        dqr = nt(cot, after)
        dke = nt(val, gf)
        dkb = dkb_s[:, sl] + nt(val, gb)
        dqb = dqb_s[:, sl]
        dkf = dkf_s[:, sl]
        eer = eer_s[0:1, sl]
        enx = enx_s[:, sl]
        en = en_s[:, sl]
        dq_ref[:, sl] = (
            (dqf * ec_s[:, sl] + (dqb + dqr * eer) * enx) * HEAD_DIM ** (-0.5)
        ).astype(BF)
        dk_ref[:, sl] = ((dkf + dke * eer) * en + dkb * ex_s[:, sl]).astype(BF)
        u1 = (
            qf_s[:, sl].astype(F32) * dqf
            - kf_s[:, sl].astype(F32) * dkf
            - ke.astype(F32) * dke
        )
        u2 = (
            kb.astype(F32) * dkb
            - qb_s[:, sl].astype(F32) * dqb
            - qr_s[:, sl].astype(F32) * dqr
        )
        cross = (ee_s[p] * f_in + sf_s[p]) * b_roll
        u_hi, u_lo = split(u1 + u2)
        c_hi, c_lo = split(cross)
        dg_ref[:, sl] = (
            nn(triu, u_hi) + nn(triu, u_lo) + nt(ones_c, c_hi) + nt(ones_c, c_lo) - u2
        ).astype(BF)
        return carry

    lax.fori_loop(0, pairs, phase_c, 0)

    own_x.wait()
    own_w.wait()
    copy_w().wait()
    for j in range(1, chips):
        copy_x(j).wait()
    xt[...] = jnp.transpose(xin[...])

    def wait_v(p, carry):
        for j in range(1, chips):
            copy_v(j, p).wait()
        return carry

    lax.fori_loop(0, pairs, wait_v, 0)

    def copy_h(c):
        return pltpu.make_async_remote_copy(
            half_out.at[c], half_in.at[c], s_h.at[c], r_h.at[c], device_id={"dp": partner})

    size = rows // chunks

    def product(side, c):
        at = pl.ds(pl.multiple_of(side * rows + c * size, size), size)
        return nn(xt[at, :], vgs[...])

    for c in range(chunks):
        half_out[c] = product(1 - core, c).astype(BF)
        copy_h(c).start()
    for c in range(chunks):
        part[c] = product(core, c)

    def copy_gf(c):
        return pltpu.make_async_remote_copy(
            gfout.at[c], gfin.at[c], s_gf.at[c], r_gf.at[c], device_id={"sp": z + 1})

    def copy_gb(c):
        return pltpu.make_async_remote_copy(
            gbout.at[c], gbin.at[c], s_gb.at[c], r_gb.at[c], device_id={"sp": z - 1})

    for c in range(chunks):
        copy_h(c).wait()
        total = part[c] + half_in[c].astype(F32)
        part[c] = total

        @pl.when(first)
        def _():
            gfout[c] = total.astype(BF)
            copy_gf(c).start()

        @pl.when(last)
        def _():
            gbout[c] = total.astype(BF)
            copy_gb(c).start()

    def sum_forward(c):
        copy_gf(c).wait_recv()

        @pl.when(z < sp - 1)
        def _():
            gfout[c] = (part[c] + gfin[c].astype(F32)).astype(BF)
            copy_gf(c).start()

    def sum_backward(c):
        copy_gb(c).wait_recv()

        @pl.when(z > 0)
        def _():
            gbout[c] = (part[c] + gbin[c].astype(F32)).astype(BF)
            copy_gb(c).start()

    @pl.when(jnp.logical_and(lower_half, z > 0))
    def _():
        for c in range(chunks):
            sum_forward(c)

    @pl.when(jnp.logical_and(jnp.logical_not(lower_half), z < sp - 1))
    def _():
        for c in range(chunks):
            sum_backward(c)

    def copy_g(j):
        other, idx = peer(j)
        return pltpu.make_async_remote_copy(
            gout.at[mine(other)], gin.at[chip], s_g.at[j], r_g.at[j], device_id={"dp": idx})

    def project(j):
        other, _ = peer(j)
        gout[mine(other), :] = nt(vgs[mine(other), :], wpair[...]).astype(BF)

    for j in range(1, chips):
        project(j)
        copy_g(j).start()
    project(0)
    gi_ref[:, chip_cols(chip)] = gout[mine(chip), :]

    @pl.when(jnp.logical_and(lower_half, z < sp - 1))
    def _():
        for c in range(chunks):
            sum_backward(c)

    @pl.when(jnp.logical_and(jnp.logical_not(lower_half), z > 0))
    def _():
        for c in range(chunks):
            sum_forward(c)

    for c in range(chunks):
        gw_ref[pl.ds(c * size, size), :] = part[c]

    @pl.when(z > 0)
    def _():
        for c in range(chunks):
            gw_ref[pl.ds(c * size, size), :] += gfin[c].astype(F32)

    @pl.when(z < sp - 1)
    def _():
        for c in range(chunks):
            gw_ref[pl.ds(c * size, size), :] += gbin[c].astype(F32)

    for j in range(1, chips):
        copy_g(j).wait()
    for j in range(1, chips):
        other, _ = peer(j)
        gi_ref[:, chip_cols(other)] = gin[other]

    @pl.when(z < sp - 1)
    def _():
        for c in range(chunks):
            copy_gf(c).wait_send()

        def drain(p, carry):
            copy_f(p).wait_send()
            return carry

        lax.fori_loop(0, pairs, drain, 0)

    @pl.when(z > 0)
    def _():
        for c in range(chunks):
            copy_gb(c).wait_send()

        def drain(p, carry):
            copy_b(p).wait_send()
            return carry

        lax.fori_loop(0, pairs, drain, 0)


def per_device(sp, dp, inputs, queries, keys, values, log_decay, cotangent, value_weight):
    tokens, model = inputs.shape[1:]
    width = queries.shape[2]
    rows = value_weight.shape[0]
    chips = dp // 2
    pairs = width // PAIR
    chunks = 4
    size = rows // chunks
    wide = lambda t: pltpu.VMEM((tokens, width), t)
    state = lambda t: pltpu.VMEM((pairs, PAIR, PAIR), t)
    dma = lambda *n: pltpu.SemaphoreType.DMA(n)
    piece = lambda t: pltpu.VMEM((chunks, size, width), t)
    outs = pl.pallas_call(
        functools.partial(kernel, sp, chips, chunks),
        out_shape=[jax.ShapeDtypeStruct((tokens, width), BF)] * 3
        + [jax.ShapeDtypeStruct((tokens, model), BF), jax.ShapeDtypeStruct((rows, width), F32)],
        in_specs=[pl.BlockSpec(memory_space=pltpu.VMEM)] * 7,
        out_specs=[pl.BlockSpec(memory_space=pltpu.VMEM)] * 5,
        scratch_shapes=[wide(BF)] * 6
        + [wide(F32)] * 4
        + [pltpu.VMEM((8, width), F32)]
        + [wide(F32)] * 5
        + [state(F32)] * 3
        + [state(BF)] * 4
        + [
            pltpu.VMEM((chips * tokens, 2 * rows), BF),
            pltpu.VMEM((2 * rows, chips * tokens), BF),
            pltpu.VMEM((chips * tokens, width), BF),
            pltpu.VMEM((2 * rows, width), BF),
            pltpu.VMEM((chips, tokens, 2 * rows), BF),
            pltpu.VMEM((chips * tokens, 2 * rows), BF),
            piece(BF), piece(BF), piece(F32), piece(BF), piece(BF), piece(BF), piece(BF),
        ]
        + [dma(pairs)] * 4
        + [dma(chips)] * 2
        + [dma(chips, pairs)] * 2
        + [pltpu.SemaphoreType.DMA] * 2
        + [dma(chips)] * 2
        + [dma(chunks)] * 6
        + [dma(2)],
        compiler_params=pltpu.CompilerParams(
            collective_id=0, has_side_effects=True, vmem_limit_bytes=60 * 1024 * 1024),
    )(inputs[0], queries[0], keys[0], values[0], log_decay[0], cotangent[0], value_weight)
    return outs[0][None], outs[1][None], outs[2][None], outs[3][None], outs[4]


def solution(mesh):
    row = P("dp", "sp", None)
    return jax.shard_map(
        functools.partial(per_device, mesh.shape["sp"], mesh.shape["dp"]),
        mesh=mesh,
        in_specs=(row,) * 6 + (P("dp", None),),
        out_specs=(row,) * 4 + (P("dp", None),),
        check_vma=False,
    )
```

```python
import functools

import jax
import jax.numpy as jnp
from jax import lax
from jax.experimental import pallas as pl
from jax.experimental.pallas import tpu as pltpu
from jax.sharding import PartitionSpec as P

HEAD_DIM = 64
PAIR = 128
BF = jnp.bfloat16
F32 = jnp.float32


def nt(a, b):
    return lax.dot_general(a, b, (((1,), (1,)), ((), ())), preferred_element_type=F32)


def nn(a, b):
    return lax.dot_general(a, b, (((1,), (0,)), ((), ())), preferred_element_type=F32)


def tn(a, b):
    return lax.dot_general(a, b, (((0,), (0,)), ((), ())), preferred_element_type=F32)


def split(a):
    hi = a.astype(BF)
    return hi, (a - hi.astype(F32)).astype(BF)


def kernel(
    sp, chips,
    x_ref, q_ref, k_ref, v_ref, g_ref, o_ref, w_ref,
    dq_ref, dk_ref, dg_ref, gi_ref, gw_ref,
    qf_s, kf_s, qb_s, kb_s, ke_s, qr_s,
    ec_s, en_s, ex_s, enx_s, eer_s,
    dqf_s, dqb_s, dkf_s, dkb_s, dv_s,
    sf_s, sb_s, ee_s,
    fin, bin_, fout, bout,
    xin, xt, vgs, wpair, gin, gout,
    half_out, half_in, part, gfin, gbin, gfout, gbout,
    s_f, r_f, s_b, r_b, s_x, r_x, s_v, r_v, s_w, r_w, s_g, r_g, s_h, r_h,
    s_gf, r_gf, s_gb, r_gb, loc,
):
    tokens, width = q_ref.shape
    pairs = width // PAIR
    rows = w_ref.shape[0]
    z = lax.axis_index("sp")
    d = lax.axis_index("dp")
    chip = d // 2
    core = lax.rem(d, 2)
    partner = chip * 2 + (1 - core)
    first = z == 0
    last = z == sp - 1
    inner = jnp.logical_and(z > 0, z < sp - 1)
    lower_half = z < sp // 2

    def peer(j):
        other = lax.rem(chip + j, chips)
        return other, other * 2 + core

    barrier = pltpu.get_barrier_semaphore()
    for j in range(1, chips):
        pl.semaphore_signal(barrier, inc=1, device_id={"dp": peer(j)[1]})
    pl.semaphore_signal(barrier, inc=1, device_id={"dp": partner})

    for step in (1, sp - 1):
        pl.semaphore_signal(barrier, inc=1, device_id={"sp": lax.rem(z + step, sp)})
    def mine(i):
        return pl.ds(pl.multiple_of(i * tokens, tokens), tokens)

    def chip_cols(i):
        return pl.ds(pl.multiple_of(i * 2 * rows, 2 * rows), 2 * rows)

    def copy_x(j):
        other, idx = peer(j)
        return pltpu.make_async_remote_copy(
            x_ref.at[:, chip_cols(other)], xin.at[mine(chip)], s_x.at[j], r_x.at[j],
            device_id={"dp": idx})

    def copy_w():
        return pltpu.make_async_remote_copy(
            w_ref, wpair.at[pl.ds(pl.multiple_of(core * rows, rows), rows)], s_w, r_w,
            device_id={"dp": partner})

    def lanes(p):
        return pl.ds(pl.multiple_of(p * PAIR, PAIR), PAIR)

    def copy_v(j, p):
        _, idx = peer(j)
        return pltpu.make_async_remote_copy(
            vgs.at[mine(chip), lanes(p)], vgs.at[mine(chip), lanes(p)],
            s_v.at[j, p], r_v.at[j, p], device_id={"dp": idx})

    def copy_f(p):
        return pltpu.make_async_remote_copy(
            fout.at[p], fin.at[p], s_f.at[p], r_f.at[p], device_id={"sp": z + 1})

    def copy_b(p):
        return pltpu.make_async_remote_copy(
            bout.at[p], bin_.at[p], s_b.at[p], r_b.at[p], device_id={"sp": z - 1})

    pl.semaphore_wait(barrier, chips + 2)

    for j in range(1, chips):
        copy_x(j).start()
    copy_w().start()
    own_x = pltpu.make_async_copy(x_ref.at[:, chip_cols(chip)], xin.at[mine(chip)], loc.at[0])
    own_x.start()
    own_w = pltpu.make_async_copy(
        w_ref, wpair.at[pl.ds(pl.multiple_of(core * rows, rows), rows)], loc.at[1])
    own_w.start()

    @pl.when(first)
    def _():
        fin[...] = jnp.zeros_like(fin)
        gfin[...] = jnp.zeros_like(gfin)

    @pl.when(last)
    def _():
        bin_[...] = jnp.zeros_like(bin_)
        gbin[...] = jnp.zeros_like(gbin)

    ti = lax.broadcasted_iota(jnp.int32, (tokens, tokens), 0)
    tj = lax.broadcasted_iota(jnp.int32, (tokens, tokens), 1)
    tril = jnp.where(tj <= ti, 1.0, 0.0).astype(BF)
    triu = jnp.where(tj >= ti, 1.0, 0.0).astype(BF)
    ci = lax.broadcasted_iota(jnp.int32, (PAIR, PAIR), 0)
    cj = lax.broadcasted_iota(jnp.int32, (PAIR, PAIR), 1)
    diag = (ci < HEAD_DIM) == (cj < HEAD_DIM)
    ones_c = jnp.ones((tokens, PAIR), BF)
    left = lax.broadcasted_iota(jnp.int32, (tokens, PAIR), 1) < HEAD_DIM
    ri = lax.broadcasted_iota(jnp.int32, (2 * tokens, tokens), 0)
    rj = lax.broadcasted_iota(jnp.int32, (2 * tokens, tokens), 1)
    rt = jnp.where(ri >= tokens, ri - tokens, ri)
    low2 = rt >= rj
    up2 = rt <= rj

    def stack(a):
        zero = jnp.zeros_like(a)
        return jnp.concatenate([jnp.where(left, a, zero), jnp.where(left, zero, a)], axis=0)

    def phase_a(p, carry):
        sl = lanes(p)
        gate = g_ref[:, sl]
        run = nn(tril, gate)
        excl = run - gate.astype(F32)
        ec = jnp.exp(run)
        en = jnp.exp(-run)
        ex = jnp.exp(excl)
        enx = jnp.exp(-excl)
        eer = ec[tokens - 1:tokens, :]
        qs = q_ref[:, sl].astype(F32) * HEAD_DIM ** (-0.5)
        ks = k_ref[:, sl].astype(F32)
        qf = (qs * ec).astype(BF)
        kb = (ks * ex).astype(BF)
        ke = (ks * (en * eer)).astype(BF)
        qr = (qs * (enx * eer)).astype(BF)
        qf_s[:, sl] = qf
        kf_s[:, sl] = (ks * en).astype(BF)
        qb_s[:, sl] = (qs * enx).astype(BF)
        kb_s[:, sl] = kb
        ke_s[:, sl] = ke
        qr_s[:, sl] = qr
        ec_s[:, sl] = ec
        en_s[:, sl] = en
        ex_s[:, sl] = ex
        enx_s[:, sl] = enx
        eer_s[:, sl] = jnp.broadcast_to(eer, (8, PAIR))
        val = v_ref[:, sl]
        cot = o_ref[:, sl]
        cot_r = pltpu.roll(cot.astype(F32), HEAD_DIM, 1).astype(BF)
        sf = jnp.where(diag, tn(ke, val), tn(qr, cot_r))
        sb = jnp.where(diag, tn(kb, val), tn(qf, cot_r))
        sf_s[p] = sf
        sb_s[p] = sb
        ee_s[p] = jnp.exp(tn(gate, ones_c))

        @pl.when(first)
        def _():
            fout[p] = sf.astype(BF)
            copy_f(p).start()

        @pl.when(last)
        def _():
            bout[p] = sb.astype(BF)
            copy_b(p).start()

        return carry

    lax.fori_loop(0, pairs, phase_a, 0)

    def forward_step(p):
        copy_f(p).wait_recv()

        @pl.when(z < sp - 1)
        def _():
            fout[p] = (ee_s[p] * fin[p].astype(F32) + sf_s[p]).astype(BF)
            copy_f(p).start()

    def backward_step(p):
        copy_b(p).wait_recv()

        @pl.when(z > 0)
        def _():
            bout[p] = (ee_s[p] * bin_[p].astype(F32) + sb_s[p]).astype(BF)
            copy_b(p).start()

    lag = pairs // 2

    def second_step(p, gate):
        @pl.when(jnp.logical_and(gate, jnp.logical_and(lower_half, z < sp - 1)))
        def _():
            backward_step(p)

        @pl.when(jnp.logical_and(gate, jnp.logical_and(jnp.logical_not(lower_half), z > 0)))
        def _():
            forward_step(p)

    def phase_b(p, carry):
        sl = lanes(p)
        qf2 = stack(qf_s[:, sl])
        qb2 = stack(qb_s[:, sl])
        cot2 = stack(o_ref[:, sl])
        kf = kf_s[:, sl]
        kb = kb_s[:, sl]
        score = jnp.where(low2, nt(qf2, kf), 0.0) + jnp.where(up2, nt(qb2, kb), 0.0)
        dscore = nt(cot2, v_ref[:, sl])
        dlow = jnp.where(low2, dscore, 0.0).astype(BF)
        dup = jnp.where(up2, dscore, 0.0).astype(BF)
        dv_s[:, sl] = tn(score.astype(BF), cot2)
        dkf_s[:, sl] = tn(dlow, qf2)
        dkb_s[:, sl] = tn(dup, qb2)
        dqf_s[:, sl] = nn(jnp.concatenate([dlow[:tokens], dlow[tokens:]], axis=1), stack(kf))
        dqb_s[:, sl] = nn(jnp.concatenate([dup[:tokens], dup[tokens:]], axis=1), stack(kb))

        @pl.when(jnp.logical_and(lower_half, z > 0))
        def _():
            forward_step(p)

        @pl.when(jnp.logical_and(jnp.logical_not(lower_half), z < sp - 1))
        def _():
            backward_step(p)

        second_step(p - lag, jnp.logical_and(inner, p >= lag))
        return carry

    lax.fori_loop(0, pairs, phase_b, 0)

    def received(p):
        f_in = fin[p].astype(F32)
        b_roll = pltpu.roll(bin_[p].astype(F32), HEAD_DIM, 1)
        gb = jnp.where(diag, pltpu.roll(f_in, HEAD_DIM, 1), 0.0).astype(BF)
        gf = jnp.where(diag, b_roll, 0.0).astype(BF)
        return f_in, b_roll, gb, gf

    def phase_v(p, carry):
        sl = lanes(p)
        second_step(p, jnp.logical_not(inner))
        second_step(p + lag, jnp.logical_and(inner, p < pairs - lag))
        _, _, gb, gf = received(p)
        dv = dv_s[:, sl] + nn(ke_s[:, sl], gf) + nn(kb_s[:, sl], gb)
        vgs[mine(chip), sl] = dv.astype(BF)
        for j in range(1, chips):
            copy_v(j, p).start()
        return carry

    lax.fori_loop(0, pairs, phase_v, 0)

    def phase_c(p):
        sl = lanes(p)
        f_in, b_roll, gb, gf = received(p)
        before = jnp.where(diag, f_in, 0.0).astype(BF)
        after = jnp.where(diag, bin_[p].astype(F32), 0.0).astype(BF)
        val = v_ref[:, sl]
        cot = o_ref[:, sl]
        ke = ke_s[:, sl]
        kb = kb_s[:, sl]
        dqf = dqf_s[:, sl] + nt(cot, before)
        dqr = nt(cot, after)
        dke = nt(val, gf)
        dkb = dkb_s[:, sl] + nt(val, gb)
        dqb = dqb_s[:, sl]
        dkf = dkf_s[:, sl]
        eer = eer_s[0:1, sl]
        enx = enx_s[:, sl]
        en = en_s[:, sl]
        dq_ref[:, sl] = (
            (dqf * ec_s[:, sl] + (dqb + dqr * eer) * enx) * HEAD_DIM ** (-0.5)
        ).astype(BF)
        dk_ref[:, sl] = ((dkf + dke * eer) * en + dkb * ex_s[:, sl]).astype(BF)
        u1 = (
            qf_s[:, sl].astype(F32) * dqf
            - kf_s[:, sl].astype(F32) * dkf
            - ke.astype(F32) * dke
        )
        u2 = (
            kb.astype(F32) * dkb
            - qb_s[:, sl].astype(F32) * dqb
            - qr_s[:, sl].astype(F32) * dqr
        )
        cross = (ee_s[p] * f_in + sf_s[p]) * b_roll
        u_hi, u_lo = split(u1 + u2)
        c_hi, c_lo = split(cross)
        dg_ref[:, sl] = (
            nn(triu, u_hi) + nn(triu, u_lo) + nt(ones_c, c_hi) + nt(ones_c, c_lo) - u2
        ).astype(BF)

    own_x.wait()
    own_w.wait()
    copy_w().wait()
    for j in range(1, chips):
        copy_x(j).wait()
    xt[...] = jnp.transpose(xin[...])

    def copy_h(p):
        return pltpu.make_async_remote_copy(
            half_out.at[p], half_in.at[p], s_h.at[p], r_h.at[p], device_id={"dp": partner})

    def copy_gf(p):
        return pltpu.make_async_remote_copy(
            gfout.at[p], gfin.at[p], s_gf.at[p], r_gf.at[p], device_id={"sp": z + 1})

    def copy_gb(p):
        return pltpu.make_async_remote_copy(
            gbout.at[p], gbin.at[p], s_gb.at[p], r_gb.at[p], device_id={"sp": z - 1})

    def product(side, p):
        at = pl.ds(pl.multiple_of(side * rows, rows), rows)
        return nn(xt[at, :], vgs[:, lanes(p)])

    def make_term(p):
        for j in range(1, chips):
            copy_v(j, p).wait()
        half_out[p] = product(1 - core, p).astype(BF)
        copy_h(p).start()
        part[p] = product(core, p)

    def join(p):
        copy_h(p).wait()
        total = part[p] + half_in[p].astype(F32)
        part[p] = total

        @pl.when(first)
        def _():
            gfout[p] = total.astype(BF)
            copy_gf(p).start()

        @pl.when(last)
        def _():
            gbout[p] = total.astype(BF)
            copy_gb(p).start()

    def sum_forward(p):
        copy_gf(p).wait_recv()

        @pl.when(z < sp - 1)
        def _():
            gfout[p] = (part[p] + gfin[p].astype(F32)).astype(BF)
            copy_gf(p).start()

    def sum_backward(p):
        copy_gb(p).wait_recv()

        @pl.when(z > 0)
        def _():
            gbout[p] = (part[p] + gbin[p].astype(F32)).astype(BF)
            copy_gb(p).start()

    def sum_step(p, lower, upper):
        within = jnp.logical_and(inner, jnp.logical_and(p >= 0, p < pairs))

        @pl.when(jnp.logical_and(within, lower_half))
        def _():
            lower(p)

        @pl.when(jnp.logical_and(within, jnp.logical_not(lower_half)))
        def _():
            upper(p)

    def pipeline(i, carry):
        @pl.when(i < pairs)
        def _():
            make_term(i)
            phase_c(i)

        @pl.when(jnp.logical_and(i >= 1, i <= pairs))
        def _():
            join(i - 1)

        sum_step(i - 3, sum_forward, sum_backward)
        sum_step(i - 5, sum_backward, sum_forward)
        return carry

    lax.fori_loop(0, pairs + 1, pipeline, 0)

    def copy_g(j):
        other, idx = peer(j)
        return pltpu.make_async_remote_copy(
            gout.at[mine(other)], gin.at[chip], s_g.at[j], r_g.at[j], device_id={"dp": idx})

    def project(j):
        other, _ = peer(j)
        gout[mine(other), :] = nt(vgs[mine(other), :], wpair[...]).astype(BF)

    for j in range(1, chips):
        project(j)
        copy_g(j).start()
    project(0)
    gi_ref[:, chip_cols(chip)] = gout[mine(chip), :]


    lax.fori_loop(pairs + 1, pairs + 5, pipeline, 0)

    def finish(p, carry):
        @pl.when(first)
        def _():
            sum_backward(p)

        @pl.when(last)
        def _():
            sum_forward(p)

        gw_ref[:, lanes(p)] = part[p] + gfin[p].astype(F32) + gbin[p].astype(F32)
        return carry

    lax.fori_loop(0, pairs, finish, 0)

    for j in range(1, chips):
        copy_g(j).wait()
    for j in range(1, chips):
        other, _ = peer(j)
        gi_ref[:, chip_cols(other)] = gin[other]

    @pl.when(z < sp - 1)
    def _():
        def drain(p, carry):
            copy_gf(p).wait_send()
            copy_f(p).wait_send()
            return carry

        lax.fori_loop(0, pairs, drain, 0)

    @pl.when(z > 0)
    def _():
        def drain(p, carry):
            copy_gb(p).wait_send()
            copy_b(p).wait_send()
            return carry

        lax.fori_loop(0, pairs, drain, 0)


def per_device(sp, dp, inputs, queries, keys, values, log_decay, cotangent, value_weight):
    tokens, model = inputs.shape[1:]
    width = queries.shape[2]
    rows = value_weight.shape[0]
    chips = dp // 2
    pairs = width // PAIR
    wide = lambda t: pltpu.VMEM((tokens, width), t)
    state = lambda t: pltpu.VMEM((pairs, PAIR, PAIR), t)
    dma = lambda *n: pltpu.SemaphoreType.DMA(n)
    piece = lambda t: pltpu.VMEM((pairs, rows, PAIR), t)
    outs = pl.pallas_call(
        functools.partial(kernel, sp, chips),
        out_shape=[jax.ShapeDtypeStruct((tokens, width), BF)] * 3
        + [jax.ShapeDtypeStruct((tokens, model), BF), jax.ShapeDtypeStruct((rows, width), F32)],
        in_specs=[pl.BlockSpec(memory_space=pltpu.VMEM)] * 7,
        out_specs=[pl.BlockSpec(memory_space=pltpu.VMEM)] * 5,
        scratch_shapes=[wide(BF)] * 6
        + [wide(F32)] * 4
        + [pltpu.VMEM((8, width), F32)]
        + [wide(F32)] * 5
        + [state(F32)] * 3
        + [state(BF)] * 4
        + [
            pltpu.VMEM((chips * tokens, 2 * rows), BF),
            pltpu.VMEM((2 * rows, chips * tokens), BF),
            pltpu.VMEM((chips * tokens, width), BF),
            pltpu.VMEM((2 * rows, width), BF),
            pltpu.VMEM((chips, tokens, 2 * rows), BF),
            pltpu.VMEM((chips * tokens, 2 * rows), BF),
            piece(BF), piece(BF), piece(F32), piece(BF), piece(BF), piece(BF), piece(BF),
        ]
        + [dma(pairs)] * 4
        + [dma(chips)] * 2
        + [dma(chips, pairs)] * 2
        + [pltpu.SemaphoreType.DMA] * 2
        + [dma(chips)] * 2
        + [dma(pairs)] * 6
        + [dma(2)],
        compiler_params=pltpu.CompilerParams(
            collective_id=0, has_side_effects=True, vmem_limit_bytes=60 * 1024 * 1024),
    )(inputs[0], queries[0], keys[0], values[0], log_decay[0], cotangent[0], value_weight)
    return outs[0][None], outs[1][None], outs[2][None], outs[3][None], outs[4]


def solution(mesh):
    row = P("dp", "sp", None)
    return jax.shard_map(
        functools.partial(per_device, mesh.shape["sp"], mesh.shape["dp"]),
        mesh=mesh,
        in_specs=(row,) * 6 + (P("dp", None),),
        out_specs=(row,) * 4 + (P("dp", None),),
        check_vma=False,
    )
```

```python
import functools

import jax
import jax.numpy as jnp
from jax import lax
from jax.experimental import pallas as pl
from jax.experimental.pallas import tpu as pltpu
from jax.sharding import PartitionSpec as P

HEAD_DIM = 64
PAIR = 128
VMEM_BYTES = 67043328
BF = jnp.bfloat16
F32 = jnp.float32


def nt(a, b):
    return lax.dot_general(a, b, (((1,), (1,)), ((), ())), preferred_element_type=F32)


def nn(a, b):
    return lax.dot_general(a, b, (((1,), (0,)), ((), ())), preferred_element_type=F32)


def tn(a, b):
    return lax.dot_general(a, b, (((0,), (0,)), ((), ())), preferred_element_type=F32)


def split(a):
    hi = a.astype(BF)
    return hi, (a - hi.astype(F32)).astype(BF)


def kernel(
    sp, chips,
    x_ref, q_in, k_in, v_in, g_in, o_in, w_ref,
    dq_ref, dk_ref, dg_ref, gi_ref, gw_ref,
    q_ref, k_ref, v_ref, g_ref, o_ref,
    qf_s, kf_s, qb_s, kb_s, ke_s, qr_s,
    ec_s, en_s, ex_s, enx_s, eer_s,
    dqf_s, dqb_s, dkf_s, dkb_s, dv_s,
    sf_s, sb_s, ee_s,
    fin, bin_, fout, bout,
    xin, xt, vgs, wpair, gin, gout,
    half_out, half_in, part, gfin, gbin, gfout, gbout,
    s_f, r_f, s_b, r_b, s_x, r_x, s_v, r_v, s_w, r_w, s_g, r_g, s_h, r_h,
    s_gf, r_gf, s_gb, r_gb, loc,
):
    tokens, width = q_ref.shape
    pairs = width // PAIR
    rows = w_ref.shape[0]
    z = lax.axis_index("sp")
    d = lax.axis_index("dp")
    chip = d // 2
    core = lax.rem(d, 2)
    partner = chip * 2 + (1 - core)
    first = z == 0
    last = z == sp - 1
    inner = jnp.logical_and(z > 0, z < sp - 1)
    lower_half = z < sp // 2

    loads = [
        pltpu.make_async_copy(a, b, loc.at[2 + i])
        for i, (a, b) in enumerate(
            ((g_in, g_ref), (q_in, q_ref), (k_in, k_ref), (v_in, v_ref), (o_in, o_ref)))
    ]
    for load in loads:
        load.start()

    def peer(j):
        other = lax.rem(chip + j, chips)
        return other, other * 2 + core

    barrier = pltpu.get_barrier_semaphore()
    for j in range(1, chips):
        pl.semaphore_signal(barrier, inc=1, device_id={"dp": peer(j)[1]})
    pl.semaphore_signal(barrier, inc=1, device_id={"dp": partner})

    for step in (1, sp - 1):
        pl.semaphore_signal(barrier, inc=1, device_id={"sp": lax.rem(z + step, sp)})
    def mine(i):
        return pl.ds(pl.multiple_of(i * tokens, tokens), tokens)

    def chip_cols(i):
        return pl.ds(pl.multiple_of(i * 2 * rows, 2 * rows), 2 * rows)

    def copy_x(j):
        other, idx = peer(j)
        return pltpu.make_async_remote_copy(
            x_ref.at[:, chip_cols(other)], xin.at[mine(chip)], s_x.at[j], r_x.at[j],
            device_id={"dp": idx})

    def copy_w():
        return pltpu.make_async_remote_copy(
            w_ref, wpair.at[pl.ds(pl.multiple_of(core * rows, rows), rows)], s_w, r_w,
            device_id={"dp": partner})

    def lanes(p):
        return pl.ds(pl.multiple_of(p * PAIR, PAIR), PAIR)

    def copy_v(j, p):
        _, idx = peer(j)
        return pltpu.make_async_remote_copy(
            vgs.at[mine(chip), lanes(p)], vgs.at[mine(chip), lanes(p)],
            s_v.at[j, p], r_v.at[j, p], device_id={"dp": idx})

    def copy_f(p):
        return pltpu.make_async_remote_copy(
            fout.at[p], fin.at[p], s_f.at[p], r_f.at[p], device_id={"sp": z + 1})

    def copy_b(p):
        return pltpu.make_async_remote_copy(
            bout.at[p], bin_.at[p], s_b.at[p], r_b.at[p], device_id={"sp": z - 1})

    pl.semaphore_wait(barrier, chips + 2)

    for j in range(1, chips):
        copy_x(j).start()
    copy_w().start()
    own_x = pltpu.make_async_copy(x_ref.at[:, chip_cols(chip)], xin.at[mine(chip)], loc.at[0])
    own_x.start()
    own_w = pltpu.make_async_copy(
        w_ref, wpair.at[pl.ds(pl.multiple_of(core * rows, rows), rows)], loc.at[1])
    own_w.start()
    for load in loads:
        load.wait()

    @pl.when(first)
    def _():
        fin[...] = jnp.zeros_like(fin)
        gfin[...] = jnp.zeros_like(gfin)

    @pl.when(last)
    def _():
        bin_[...] = jnp.zeros_like(bin_)
        gbin[...] = jnp.zeros_like(gbin)

    ti = lax.broadcasted_iota(jnp.int32, (tokens, tokens), 0)
    tj = lax.broadcasted_iota(jnp.int32, (tokens, tokens), 1)
    tril = jnp.where(tj <= ti, 1.0, 0.0).astype(BF)
    triu = jnp.where(tj >= ti, 1.0, 0.0).astype(BF)
    ci = lax.broadcasted_iota(jnp.int32, (PAIR, PAIR), 0)
    cj = lax.broadcasted_iota(jnp.int32, (PAIR, PAIR), 1)
    diag = (ci < HEAD_DIM) == (cj < HEAD_DIM)
    ones_c = jnp.ones((tokens, PAIR), BF)
    left = lax.broadcasted_iota(jnp.int32, (tokens, PAIR), 1) < HEAD_DIM
    ri = lax.broadcasted_iota(jnp.int32, (2 * tokens, tokens), 0)
    rj = lax.broadcasted_iota(jnp.int32, (2 * tokens, tokens), 1)
    rt = jnp.where(ri >= tokens, ri - tokens, ri)
    low2 = rt >= rj
    up2 = rt <= rj

    def stack(a):
        zero = jnp.zeros_like(a)
        return jnp.concatenate([jnp.where(left, a, zero), jnp.where(left, zero, a)], axis=0)

    def phase_a(p, carry):
        sl = lanes(p)
        gate = g_ref[:, sl]
        run = nn(tril, gate)
        excl = run - gate.astype(F32)
        ec = jnp.exp(run)
        en = jnp.exp(-run)
        ex = jnp.exp(excl)
        enx = jnp.exp(-excl)
        eer = ec[tokens - 1:tokens, :]
        qs = q_ref[:, sl].astype(F32) * HEAD_DIM ** (-0.5)
        ks = k_ref[:, sl].astype(F32)
        qf = (qs * ec).astype(BF)
        kb = (ks * ex).astype(BF)
        ke = (ks * (en * eer)).astype(BF)
        qr = (qs * (enx * eer)).astype(BF)
        qf_s[:, sl] = qf
        kf_s[:, sl] = (ks * en).astype(BF)
        qb_s[:, sl] = (qs * enx).astype(BF)
        kb_s[:, sl] = kb
        ke_s[:, sl] = ke
        qr_s[:, sl] = qr
        ec_s[:, sl] = ec
        en_s[:, sl] = en
        ex_s[:, sl] = ex
        enx_s[:, sl] = enx
        eer_s[:, sl] = jnp.broadcast_to(eer, (8, PAIR))
        val = v_ref[:, sl]
        cot = o_ref[:, sl]
        cot_r = pltpu.roll(cot.astype(F32), HEAD_DIM, 1).astype(BF)
        sf = jnp.where(diag, tn(ke, val), tn(qr, cot_r))
        sb = jnp.where(diag, tn(kb, val), tn(qf, cot_r))
        sf_s[p] = sf
        sb_s[p] = sb
        ee_s[p] = jnp.exp(tn(gate, ones_c))

        @pl.when(first)
        def _():
            fout[p] = sf.astype(BF)
            copy_f(p).start()

        @pl.when(last)
        def _():
            bout[p] = sb.astype(BF)
            copy_b(p).start()

        return carry

    lax.fori_loop(0, pairs, phase_a, 0)

    def forward_step(p):
        copy_f(p).wait_recv()

        @pl.when(z < sp - 1)
        def _():
            fout[p] = (ee_s[p] * fin[p].astype(F32) + sf_s[p]).astype(BF)
            copy_f(p).start()

    def backward_step(p):
        copy_b(p).wait_recv()

        @pl.when(z > 0)
        def _():
            bout[p] = (ee_s[p] * bin_[p].astype(F32) + sb_s[p]).astype(BF)
            copy_b(p).start()

    lag = pairs // 2

    def second_step(p, gate):
        @pl.when(jnp.logical_and(gate, jnp.logical_and(lower_half, z < sp - 1)))
        def _():
            backward_step(p)

        @pl.when(jnp.logical_and(gate, jnp.logical_and(jnp.logical_not(lower_half), z > 0)))
        def _():
            forward_step(p)

    def phase_b(p, carry):
        sl = lanes(p)
        qf2 = stack(qf_s[:, sl])
        qb2 = stack(qb_s[:, sl])
        cot2 = stack(o_ref[:, sl])
        kf = kf_s[:, sl]
        kb = kb_s[:, sl]
        score = jnp.where(low2, nt(qf2, kf), 0.0) + jnp.where(up2, nt(qb2, kb), 0.0)
        dscore = nt(cot2, v_ref[:, sl])
        dlow = jnp.where(low2, dscore, 0.0).astype(BF)
        dup = jnp.where(up2, dscore, 0.0).astype(BF)
        dv_s[:, sl] = tn(score.astype(BF), cot2)
        dkf_s[:, sl] = tn(dlow, qf2)
        dkb_s[:, sl] = tn(dup, qb2)
        dqf_s[:, sl] = nn(jnp.concatenate([dlow[:tokens], dlow[tokens:]], axis=1), stack(kf))
        dqb_s[:, sl] = nn(jnp.concatenate([dup[:tokens], dup[tokens:]], axis=1), stack(kb))

        @pl.when(jnp.logical_and(lower_half, z > 0))
        def _():
            forward_step(p)

        @pl.when(jnp.logical_and(jnp.logical_not(lower_half), z < sp - 1))
        def _():
            backward_step(p)

        second_step(p - lag, jnp.logical_and(inner, p >= lag))
        return carry

    lax.fori_loop(0, pairs, phase_b, 0)

    def received(p):
        f_in = fin[p].astype(F32)
        b_roll = pltpu.roll(bin_[p].astype(F32), HEAD_DIM, 1)
        gb = jnp.where(diag, pltpu.roll(f_in, HEAD_DIM, 1), 0.0).astype(BF)
        gf = jnp.where(diag, b_roll, 0.0).astype(BF)
        return f_in, b_roll, gb, gf

    def phase_v(p, carry):
        sl = lanes(p)
        second_step(p, jnp.logical_not(inner))
        second_step(p + lag, jnp.logical_and(inner, p < pairs - lag))
        _, _, gb, gf = received(p)
        dv = dv_s[:, sl] + nn(ke_s[:, sl], gf) + nn(kb_s[:, sl], gb)
        vgs[mine(chip), sl] = dv.astype(BF)
        for j in range(1, chips):
            copy_v(j, p).start()
        return carry

    lax.fori_loop(0, pairs, phase_v, 0)

    def phase_c(p):
        sl = lanes(p)
        f_in, b_roll, gb, gf = received(p)
        before = jnp.where(diag, f_in, 0.0).astype(BF)
        after = jnp.where(diag, bin_[p].astype(F32), 0.0).astype(BF)
        val = v_ref[:, sl]
        cot = o_ref[:, sl]
        ke = ke_s[:, sl]
        kb = kb_s[:, sl]
        dqf = dqf_s[:, sl] + nt(cot, before)
        dqr = nt(cot, after)
        dke = nt(val, gf)
        dkb = dkb_s[:, sl] + nt(val, gb)
        dqb = dqb_s[:, sl]
        dkf = dkf_s[:, sl]
        eer = eer_s[0:1, sl]
        enx = enx_s[:, sl]
        en = en_s[:, sl]
        dq_ref[:, sl] = (
            (dqf * ec_s[:, sl] + (dqb + dqr * eer) * enx) * HEAD_DIM ** (-0.5)
        ).astype(BF)
        dk_ref[:, sl] = ((dkf + dke * eer) * en + dkb * ex_s[:, sl]).astype(BF)
        u1 = (
            qf_s[:, sl].astype(F32) * dqf
            - kf_s[:, sl].astype(F32) * dkf
            - ke.astype(F32) * dke
        )
        u2 = (
            kb.astype(F32) * dkb
            - qb_s[:, sl].astype(F32) * dqb
            - qr_s[:, sl].astype(F32) * dqr
        )
        cross = (ee_s[p] * f_in + sf_s[p]) * b_roll
        u_hi, u_lo = split(u1 + u2)
        c_hi, c_lo = split(cross)
        dg_ref[:, sl] = (
            nn(triu, u_hi) + nn(triu, u_lo) + nt(ones_c, c_hi) + nt(ones_c, c_lo) - u2
        ).astype(BF)

    own_x.wait()
    own_w.wait()
    copy_w().wait()
    for j in range(1, chips):
        copy_x(j).wait()
    xt[...] = jnp.transpose(xin[...])

    def copy_h(p):
        return pltpu.make_async_remote_copy(
            half_out.at[p], half_in.at[p], s_h.at[p], r_h.at[p], device_id={"dp": partner})

    def copy_gf(p):
        return pltpu.make_async_remote_copy(
            gfout.at[p], gfin.at[p], s_gf.at[p], r_gf.at[p], device_id={"sp": z + 1})

    def copy_gb(p):
        return pltpu.make_async_remote_copy(
            gbout.at[p], gbin.at[p], s_gb.at[p], r_gb.at[p], device_id={"sp": z - 1})

    def product(side, p):
        at = pl.ds(pl.multiple_of(side * rows, rows), rows)
        return nn(xt[at, :], vgs[:, lanes(p)])

    def make_term(p):
        for j in range(1, chips):
            copy_v(j, p).wait()
        half_out[p] = product(1 - core, p).astype(BF)
        copy_h(p).start()
        part[p] = product(core, p)

    def join(p):
        copy_h(p).wait()
        total = part[p] + half_in[p].astype(F32)
        part[p] = total

        @pl.when(first)
        def _():
            gfout[p] = total.astype(BF)
            copy_gf(p).start()

        @pl.when(last)
        def _():
            gbout[p] = total.astype(BF)
            copy_gb(p).start()

    def sum_forward(p):
        copy_gf(p).wait_recv()

        @pl.when(z < sp - 1)
        def _():
            gfout[p] = (part[p] + gfin[p].astype(F32)).astype(BF)
            copy_gf(p).start()

    def sum_backward(p):
        copy_gb(p).wait_recv()

        @pl.when(z > 0)
        def _():
            gbout[p] = (part[p] + gbin[p].astype(F32)).astype(BF)
            copy_gb(p).start()

    def sum_step(p, lower, upper):
        within = jnp.logical_and(inner, jnp.logical_and(p >= 0, p < pairs))

        @pl.when(jnp.logical_and(within, lower_half))
        def _():
            lower(p)

        @pl.when(jnp.logical_and(within, jnp.logical_not(lower_half)))
        def _():
            upper(p)

    def pipeline(i, carry):
        @pl.when(i < pairs)
        def _():
            make_term(i)
            phase_c(i)

        @pl.when(jnp.logical_and(i >= 1, i <= pairs))
        def _():
            join(i - 1)

        sum_step(i - 3, sum_forward, sum_backward)
        sum_step(i - 5, sum_backward, sum_forward)
        return carry

    lax.fori_loop(0, pairs + 1, pipeline, 0)

    def copy_g(j):
        other, idx = peer(j)
        return pltpu.make_async_remote_copy(
            gout.at[mine(other)], gin.at[chip], s_g.at[j], r_g.at[j], device_id={"dp": idx})

    def project(j):
        other, _ = peer(j)
        gout[mine(other), :] = nt(vgs[mine(other), :], wpair[...]).astype(BF)

    for j in range(1, chips):
        project(j)
        copy_g(j).start()
    project(0)
    gi_ref[:, chip_cols(chip)] = gout[mine(chip), :]


    lax.fori_loop(pairs + 1, pairs + 5, pipeline, 0)

    def finish(p, carry):
        @pl.when(first)
        def _():
            sum_backward(p)

        @pl.when(last)
        def _():
            sum_forward(p)

        gw_ref[:, lanes(p)] = part[p] + gfin[p].astype(F32) + gbin[p].astype(F32)
        return carry

    lax.fori_loop(0, pairs, finish, 0)

    for j in range(1, chips):
        copy_g(j).wait()
    for j in range(1, chips):
        other, _ = peer(j)
        gi_ref[:, chip_cols(other)] = gin[other]

    @pl.when(z < sp - 1)
    def _():
        def drain(p, carry):
            copy_gf(p).wait_send()
            copy_f(p).wait_send()
            return carry

        lax.fori_loop(0, pairs, drain, 0)

    @pl.when(z > 0)
    def _():
        def drain(p, carry):
            copy_gb(p).wait_send()
            copy_b(p).wait_send()
            return carry

        lax.fori_loop(0, pairs, drain, 0)


def write_out(*refs):
    sems = refs[10]
    copies = [
        pltpu.make_async_copy(refs[i], refs[5 + i], sems.at[i]) for i in (4, 3, 0, 1, 2)
    ]
    for copy in copies:
        copy.start()
    for copy in copies:
        copy.wait()


def per_device(sp, dp, inputs, queries, keys, values, log_decay, cotangent, value_weight):
    tokens, model = inputs.shape[1:]
    width = queries.shape[2]
    rows = value_weight.shape[0]
    chips = dp // 2
    pairs = width // PAIR
    wide = lambda t: pltpu.VMEM((tokens, width), t)
    state = lambda t: pltpu.VMEM((pairs, PAIR, PAIR), t)
    dma = lambda *n: pltpu.SemaphoreType.DMA(n)
    piece = lambda t: pltpu.VMEM((pairs, rows, PAIR), t)
    shapes = [jax.ShapeDtypeStruct((tokens, width), BF)] * 3
    shapes += [jax.ShapeDtypeStruct((tokens, model), BF), jax.ShapeDtypeStruct((rows, width), F32)]
    kept = sum(a.size * a.dtype.itemsize for a in shapes) + 64 * 1024
    outs = pl.pallas_call(
        functools.partial(kernel, sp, chips),
        out_shape=[pltpu.VMEM(a.shape, a.dtype) for a in shapes],
        in_specs=[pl.BlockSpec(memory_space=pltpu.MemorySpace.HBM)] * 7,
        out_specs=[pl.BlockSpec(memory_space=pltpu.VMEM)] * 5,
        scratch_shapes=[wide(BF)] * 11
        + [wide(F32)] * 4
        + [pltpu.VMEM((8, width), F32)]
        + [wide(F32)] * 5
        + [state(F32)] * 3
        + [state(BF)] * 4
        + [
            pltpu.VMEM((chips * tokens, 2 * rows), BF),
            pltpu.VMEM((2 * rows, chips * tokens), BF),
            pltpu.VMEM((chips * tokens, width), BF),
            pltpu.VMEM((2 * rows, width), BF),
            pltpu.VMEM((chips, tokens, 2 * rows), BF),
            pltpu.VMEM((chips * tokens, 2 * rows), BF),
            piece(BF), piece(BF), piece(F32), piece(BF), piece(BF), piece(BF), piece(BF),
        ]
        + [dma(pairs)] * 4
        + [dma(chips)] * 2
        + [dma(chips, pairs)] * 2
        + [pltpu.SemaphoreType.DMA] * 2
        + [dma(chips)] * 2
        + [dma(pairs)] * 6
        + [dma(7)],
        compiler_params=pltpu.CompilerParams(
            collective_id=0, has_side_effects=True, vmem_limit_bytes=VMEM_BYTES - kept),
    )(inputs[0], queries[0], keys[0], values[0], log_decay[0], cotangent[0], value_weight)
    outs = pl.pallas_call(
        write_out,
        out_shape=shapes,
        in_specs=[pl.BlockSpec(memory_space=pl.ANY)] * 5,
        out_specs=[pl.BlockSpec(memory_space=pl.ANY)] * 5,
        scratch_shapes=[dma(5)],
        compiler_params=pltpu.CompilerParams(vmem_limit_bytes=1024 * 1024),
    )(*outs)
    return outs[0][None], outs[1][None], outs[2][None], outs[3][None], outs[4]


def solution(mesh):
    row = P("dp", "sp", None)
    return jax.shard_map(
        functools.partial(per_device, mesh.shape["sp"], mesh.shape["dp"]),
        mesh=mesh,
        in_specs=(row,) * 6 + (P("dp", None),),
        out_specs=(row,) * 4 + (P("dp", None),),
        check_vma=False,
    )
```

```python
import functools

import jax
import jax.numpy as jnp
from jax import lax
from jax.experimental import pallas as pl
from jax.experimental.pallas import tpu as pltpu
from jax.sharding import PartitionSpec as P

HEAD_DIM = 64
PAIR = 128
VMEM_BYTES = 67043328
BF = jnp.bfloat16
F32 = jnp.float32


def nt(a, b):
    return lax.dot_general(a, b, (((1,), (1,)), ((), ())), preferred_element_type=F32)


def nn(a, b):
    return lax.dot_general(a, b, (((1,), (0,)), ((), ())), preferred_element_type=F32)


def tn(a, b):
    return lax.dot_general(a, b, (((0,), (0,)), ((), ())), preferred_element_type=F32)


def split(a):
    hi = a.astype(BF)
    return hi, (a - hi.astype(F32)).astype(BF)


def kernel(
    sp, chips,
    x_ref, q_in, k_in, v_in, g_in, o_in, w_ref,
    dq_ref, dk_ref, dg_ref, gi_ref, gw_ref,
    q_ref, k_ref, v_ref, g_ref, o_ref,
    qf_s, kf_s, qb_s, kb_s, ke_s, qr_s,
    ec_s, en_s, ex_s, enx_s, eer_s,
    dqf_s, dqb_s, dkf_s, dkb_s, dv_s,
    sf_s, sb_s, ee_s,
    fin, bin_, fout, bout,
    xin, xt, vgs, wpair, gout,
    half_out, half_in, part, gfin, gbin, gfout, gbout,
    s_f, r_f, s_b, r_b, s_x, r_x, s_v, r_v, s_w, r_w, s_g, r_g, s_h, r_h,
    s_gf, r_gf, s_gb, r_gb, loc,
):
    tokens, width = q_ref.shape
    pairs = width // PAIR
    rows = w_ref.shape[0]
    z = lax.axis_index("sp")
    d = lax.axis_index("dp")
    chip = d // 2
    core = lax.rem(d, 2)
    partner = chip * 2 + (1 - core)
    first = z == 0
    last = z == sp - 1
    inner = jnp.logical_and(z > 0, z < sp - 1)
    lower_half = z < sp // 2

    loads = [
        pltpu.make_async_copy(a, b, loc.at[2 + i])
        for i, (a, b) in enumerate(
            ((g_in, g_ref), (q_in, q_ref), (k_in, k_ref), (v_in, v_ref), (o_in, o_ref)))
    ]
    for load in loads:
        load.start()

    def peer(j):
        other = lax.rem(chip + j, chips)
        return other, other * 2 + core

    barrier = pltpu.get_barrier_semaphore()
    for j in range(1, chips):
        pl.semaphore_signal(barrier, inc=1, device_id={"dp": peer(j)[1]})
    pl.semaphore_signal(barrier, inc=1, device_id={"dp": partner})

    for step in (1, sp - 1):
        pl.semaphore_signal(barrier, inc=1, device_id={"sp": lax.rem(z + step, sp)})
    def mine(i):
        return pl.ds(pl.multiple_of(i * tokens, tokens), tokens)

    def chip_cols(i):
        return pl.ds(pl.multiple_of(i * 2 * rows, 2 * rows), 2 * rows)

    def copy_x(j):
        other, idx = peer(j)
        return pltpu.make_async_remote_copy(
            x_ref.at[:, chip_cols(other)], xin.at[mine(chip)], s_x.at[j], r_x.at[j],
            device_id={"dp": idx})

    def copy_w():
        return pltpu.make_async_remote_copy(
            w_ref, wpair.at[pl.ds(pl.multiple_of(core * rows, rows), rows)], s_w, r_w,
            device_id={"dp": partner})

    def lanes(p):
        return pl.ds(pl.multiple_of(p * PAIR, PAIR), PAIR)

    def copy_v(j, p):
        _, idx = peer(j)
        return pltpu.make_async_remote_copy(
            vgs.at[mine(chip), lanes(p)], vgs.at[mine(chip), lanes(p)],
            s_v.at[j, p], r_v.at[j, p], device_id={"dp": idx})

    def copy_f(p):
        return pltpu.make_async_remote_copy(
            fout.at[p], fin.at[p], s_f.at[p], r_f.at[p], device_id={"sp": z + 1})

    def copy_b(p):
        return pltpu.make_async_remote_copy(
            bout.at[p], bin_.at[p], s_b.at[p], r_b.at[p], device_id={"sp": z - 1})

    pl.semaphore_wait(barrier, chips + 2)

    for j in range(1, chips):
        copy_x(j).start()
    copy_w().start()
    own_x = pltpu.make_async_copy(x_ref.at[:, chip_cols(chip)], xin.at[mine(chip)], loc.at[0])
    own_x.start()
    own_w = pltpu.make_async_copy(
        w_ref, wpair.at[pl.ds(pl.multiple_of(core * rows, rows), rows)], loc.at[1])
    own_w.start()
    for load in loads:
        load.wait()

    @pl.when(first)
    def _():
        fin[...] = jnp.zeros_like(fin)
        gfin[...] = jnp.zeros_like(gfin)

    @pl.when(last)
    def _():
        bin_[...] = jnp.zeros_like(bin_)
        gbin[...] = jnp.zeros_like(gbin)

    ti = lax.broadcasted_iota(jnp.int32, (tokens, tokens), 0)
    tj = lax.broadcasted_iota(jnp.int32, (tokens, tokens), 1)
    tril = jnp.where(tj <= ti, 1.0, 0.0).astype(BF)
    triu = jnp.where(tj >= ti, 1.0, 0.0).astype(BF)
    ci = lax.broadcasted_iota(jnp.int32, (PAIR, PAIR), 0)
    cj = lax.broadcasted_iota(jnp.int32, (PAIR, PAIR), 1)
    diag = (ci < HEAD_DIM) == (cj < HEAD_DIM)
    ones_c = jnp.ones((tokens, PAIR), BF)
    left = lax.broadcasted_iota(jnp.int32, (tokens, PAIR), 1) < HEAD_DIM
    ri = lax.broadcasted_iota(jnp.int32, (2 * tokens, tokens), 0)
    rj = lax.broadcasted_iota(jnp.int32, (2 * tokens, tokens), 1)
    rt = jnp.where(ri >= tokens, ri - tokens, ri)
    low2 = rt >= rj
    up2 = rt <= rj

    def stack(a):
        zero = jnp.zeros_like(a)
        return jnp.concatenate([jnp.where(left, a, zero), jnp.where(left, zero, a)], axis=0)

    def phase_a(p):
        sl = lanes(p)
        gate = g_ref[:, sl]
        run = nn(tril, gate)
        excl = run - gate.astype(F32)
        ec = jnp.exp(run)
        en = jnp.exp(-run)
        ex = jnp.exp(excl)
        enx = jnp.exp(-excl)
        eer = ec[tokens - 1:tokens, :]
        qs = q_ref[:, sl].astype(F32) * HEAD_DIM ** (-0.5)
        ks = k_ref[:, sl].astype(F32)
        qf = (qs * ec).astype(BF)
        kb = (ks * ex).astype(BF)
        ke = (ks * (en * eer)).astype(BF)
        qr = (qs * (enx * eer)).astype(BF)
        qf_s[:, sl] = qf
        kf_s[:, sl] = (ks * en).astype(BF)
        qb_s[:, sl] = (qs * enx).astype(BF)
        kb_s[:, sl] = kb
        ke_s[:, sl] = ke
        qr_s[:, sl] = qr
        ec_s[:, sl] = ec
        en_s[:, sl] = en
        ex_s[:, sl] = ex
        enx_s[:, sl] = enx
        eer_s[:, sl] = jnp.broadcast_to(eer, (8, PAIR))
        val = v_ref[:, sl]
        cot = o_ref[:, sl]
        cot_r = pltpu.roll(cot.astype(F32), HEAD_DIM, 1).astype(BF)
        sf = jnp.where(diag, tn(ke, val), tn(qr, cot_r))
        sb = jnp.where(diag, tn(kb, val), tn(qf, cot_r))
        sf_s[p] = sf
        sb_s[p] = sb
        ee_s[p] = jnp.exp(tn(gate, ones_c))

    group = 2 if pairs % 2 == 0 else 1

    def phase_a_loop(i, carry):
        for n in range(group):
            phase_a(i * group + n)

        @pl.when(first)
        def _():
            for n in range(group):
                p = i * group + n
                fout[p] = sf_s[p].astype(BF)
                copy_f(p).start()

        @pl.when(last)
        def _():
            for n in range(group):
                p = i * group + n
                bout[p] = sb_s[p].astype(BF)
                copy_b(p).start()

        return carry

    lax.fori_loop(0, pairs // group, phase_a_loop, 0)

    def forward_step(p):
        copy_f(p).wait_recv()

        @pl.when(z < sp - 1)
        def _():
            fout[p] = (ee_s[p] * fin[p].astype(F32) + sf_s[p]).astype(BF)
            copy_f(p).start()

    def backward_step(p):
        copy_b(p).wait_recv()

        @pl.when(z > 0)
        def _():
            bout[p] = (ee_s[p] * bin_[p].astype(F32) + sb_s[p]).astype(BF)
            copy_b(p).start()

    lag = pairs // 2

    def second_step(p, gate):
        @pl.when(jnp.logical_and(gate, jnp.logical_and(lower_half, z < sp - 1)))
        def _():
            backward_step(p)

        @pl.when(jnp.logical_and(gate, jnp.logical_and(jnp.logical_not(lower_half), z > 0)))
        def _():
            forward_step(p)

    def phase_b(p):
        sl = lanes(p)
        qf2 = stack(qf_s[:, sl])
        qb2 = stack(qb_s[:, sl])
        cot2 = stack(o_ref[:, sl])
        kf = kf_s[:, sl]
        kb = kb_s[:, sl]
        score = jnp.where(low2, nt(qf2, kf), 0.0) + jnp.where(up2, nt(qb2, kb), 0.0)
        dscore = nt(cot2, v_ref[:, sl])
        dlow = jnp.where(low2, dscore, 0.0).astype(BF)
        dup = jnp.where(up2, dscore, 0.0).astype(BF)
        dv_s[:, sl] = tn(score.astype(BF), cot2)
        dkf_s[:, sl] = tn(dlow, qf2)
        dkb_s[:, sl] = tn(dup, qb2)
        dqf_s[:, sl] = nn(jnp.concatenate([dlow[:tokens], dlow[tokens:]], axis=1), stack(kf))
        dqb_s[:, sl] = nn(jnp.concatenate([dup[:tokens], dup[tokens:]], axis=1), stack(kb))

    def phase_b_loop(i, carry):
        for n in range(group):
            phase_b(i * group + n)
        for n in range(group):
            p = i * group + n

            @pl.when(jnp.logical_and(lower_half, z > 0))
            def _():
                forward_step(p)

            @pl.when(jnp.logical_and(jnp.logical_not(lower_half), z < sp - 1))
            def _():
                backward_step(p)

            second_step(p - lag, jnp.logical_and(inner, p >= lag))
        return carry

    lax.fori_loop(0, pairs // group, phase_b_loop, 0)

    def received(p):
        f_in = fin[p].astype(F32)
        b_roll = pltpu.roll(bin_[p].astype(F32), HEAD_DIM, 1)
        gb = jnp.where(diag, pltpu.roll(f_in, HEAD_DIM, 1), 0.0).astype(BF)
        gf = jnp.where(diag, b_roll, 0.0).astype(BF)
        return f_in, b_roll, gb, gf

    def phase_v(p):
        sl = lanes(p)
        second_step(p, jnp.logical_not(inner))
        second_step(p + lag, jnp.logical_and(inner, p < pairs - lag))
        _, _, gb, gf = received(p)
        dv = dv_s[:, sl] + nn(ke_s[:, sl], gf) + nn(kb_s[:, sl], gb)
        vgs[mine(chip), sl] = dv.astype(BF)
        for j in range(1, chips):
            copy_v(j, p).start()

    def phase_v_loop(p, carry):
        @pl.when(jnp.logical_or(inner, p < lag))
        def _():
            phase_v(p)

        return carry

    lax.fori_loop(0, pairs, phase_v_loop, 0)

    def phase_c(p):
        sl = lanes(p)
        f_in, b_roll, gb, gf = received(p)
        before = jnp.where(diag, f_in, 0.0).astype(BF)
        after = jnp.where(diag, bin_[p].astype(F32), 0.0).astype(BF)
        val = v_ref[:, sl]
        cot = o_ref[:, sl]
        ke = ke_s[:, sl]
        kb = kb_s[:, sl]
        dqf = dqf_s[:, sl] + nt(cot, before)
        dqr = nt(cot, after)
        dke = nt(val, gf)
        dkb = dkb_s[:, sl] + nt(val, gb)
        dqb = dqb_s[:, sl]
        dkf = dkf_s[:, sl]
        eer = eer_s[0:1, sl]
        enx = enx_s[:, sl]
        en = en_s[:, sl]
        dq_ref[:, sl] = (
            (dqf * ec_s[:, sl] + (dqb + dqr * eer) * enx) * HEAD_DIM ** (-0.5)
        ).astype(BF)
        dk_ref[:, sl] = ((dkf + dke * eer) * en + dkb * ex_s[:, sl]).astype(BF)
        u1 = (
            qf_s[:, sl].astype(F32) * dqf
            - kf_s[:, sl].astype(F32) * dkf
            - ke.astype(F32) * dke
        )
        u2 = (
            kb.astype(F32) * dkb
            - qb_s[:, sl].astype(F32) * dqb
            - qr_s[:, sl].astype(F32) * dqr
        )
        cross = (ee_s[p] * f_in + sf_s[p]) * b_roll
        u_hi, u_lo = split(u1 + u2)
        c_hi, c_lo = split(cross)
        dg_ref[:, sl] = (
            nn(triu, u_hi) + nn(triu, u_lo) + nt(ones_c, c_hi) + nt(ones_c, c_lo) - u2
        ).astype(BF)

    own_x.wait()
    own_w.wait()
    copy_w().wait()
    for j in range(1, chips):
        copy_x(j).wait()
    xt[...] = jnp.transpose(xin[...])

    def copy_h(p):
        return pltpu.make_async_remote_copy(
            half_out.at[p], half_in.at[p], s_h.at[p], r_h.at[p], device_id={"dp": partner})

    def copy_gf(p):
        return pltpu.make_async_remote_copy(
            gfout.at[p], gfin.at[p], s_gf.at[p], r_gf.at[p], device_id={"sp": z + 1})

    def copy_gb(p):
        return pltpu.make_async_remote_copy(
            gbout.at[p], gbin.at[p], s_gb.at[p], r_gb.at[p], device_id={"sp": z - 1})

    def product(side, p):
        at = pl.ds(pl.multiple_of(side * rows, rows), rows)
        return nn(xt[at, :], vgs[:, lanes(p)])

    def make_term(p):
        for j in range(1, chips):
            copy_v(j, p).wait()
        half_out[p] = product(1 - core, p).astype(BF)
        copy_h(p).start()
        part[p] = product(core, p)

    def join(p):
        copy_h(p).wait()
        total = part[p] + half_in[p].astype(F32)
        part[p] = total

        @pl.when(first)
        def _():
            gfout[p] = total.astype(BF)
            copy_gf(p).start()

        @pl.when(last)
        def _():
            gbout[p] = total.astype(BF)
            copy_gb(p).start()

    def sum_forward(p):
        copy_gf(p).wait_recv()

        @pl.when(z < sp - 1)
        def _():
            gfout[p] = (part[p] + gfin[p].astype(F32)).astype(BF)
            copy_gf(p).start()

    def sum_backward(p):
        copy_gb(p).wait_recv()

        @pl.when(z > 0)
        def _():
            gbout[p] = (part[p] + gbin[p].astype(F32)).astype(BF)
            copy_gb(p).start()

    def sum_step(p, lower, upper):
        within = inner
        if not isinstance(p, int):
            within = jnp.logical_and(inner, jnp.logical_and(p >= 0, p < pairs))

        @pl.when(jnp.logical_and(within, lower_half))
        def _():
            lower(p)

        @pl.when(jnp.logical_and(within, jnp.logical_not(lower_half)))
        def _():
            upper(p)

    def pipeline(i, carry):
        @pl.when(jnp.logical_and(jnp.logical_not(inner), i < pairs - lag))
        def _():
            phase_v(i + lag)

        @pl.when(i < pairs)
        def _():
            make_term(i)

        @pl.when(jnp.logical_and(i >= 1, i <= pairs))
        def _():
            join(i - 1)

        sum_step(i - 2, sum_forward, sum_backward)
        sum_step(i - 4, sum_backward, sum_forward)

        @pl.when(i < pairs)
        def _():
            phase_c(i)

        return carry

    lax.fori_loop(0, pairs + 1, pipeline, 0)

    def copy_g(j):
        other, idx = peer(j)
        return pltpu.make_async_remote_copy(
            gout.at[mine(other)], gi_ref.at[:, chip_cols(chip)], s_g.at[j], r_g.at[j], device_id={"dp": idx})

    def project(j):
        other, _ = peer(j)
        gout[mine(other), :] = nt(vgs[mine(other), :], wpair[...]).astype(BF)

    def project_to(j):
        project(j)
        if j:
            copy_g(j).start()

    sum_step(pairs - 1, sum_forward, sum_backward)
    project_to(1)
    sum_step(pairs - 3, sum_backward, sum_forward)
    for j in range(2, chips - 1):
        project_to(j)
    sum_step(pairs - 2, sum_backward, sum_forward)
    project_to(chips - 1)
    sum_step(pairs - 1, sum_backward, sum_forward)
    project(0)
    gi_ref[:, chip_cols(chip)] = gout[mine(chip), :]

    def finish(p, carry):
        @pl.when(first)
        def _():
            sum_backward(p)

        @pl.when(last)
        def _():
            sum_forward(p)

        gw_ref[:, lanes(p)] = part[p] + gfin[p].astype(F32) + gbin[p].astype(F32)
        return carry

    lax.fori_loop(0, pairs, finish, 0)

    for j in range(1, chips):
        copy_g(j).wait()

    @pl.when(z < sp - 1)
    def _():
        def drain(p, carry):
            copy_gf(p).wait_send()
            copy_f(p).wait_send()
            return carry

        lax.fori_loop(0, pairs, drain, 0)

    @pl.when(z > 0)
    def _():
        def drain(p, carry):
            copy_gb(p).wait_send()
            copy_b(p).wait_send()
            return carry

        lax.fori_loop(0, pairs, drain, 0)


def write_out(*refs):
    sems = refs[10]
    copies = [
        pltpu.make_async_copy(refs[i], refs[5 + i], sems.at[i]) for i in (4, 3, 0, 1, 2)
    ]
    for copy in copies:
        copy.start()
    for copy in copies:
        copy.wait()


def per_device(sp, dp, inputs, queries, keys, values, log_decay, cotangent, value_weight):
    tokens, model = inputs.shape[1:]
    width = queries.shape[2]
    rows = value_weight.shape[0]
    chips = dp // 2
    pairs = width // PAIR
    wide = lambda t: pltpu.VMEM((tokens, width), t)
    state = lambda t: pltpu.VMEM((pairs, PAIR, PAIR), t)
    dma = lambda *n: pltpu.SemaphoreType.DMA(n)
    piece = lambda t: pltpu.VMEM((pairs, rows, PAIR), t)
    shapes = [jax.ShapeDtypeStruct((tokens, width), BF)] * 3
    shapes += [jax.ShapeDtypeStruct((tokens, model), BF), jax.ShapeDtypeStruct((rows, width), F32)]
    kept = sum(a.size * a.dtype.itemsize for a in shapes) + 64 * 1024
    outs = pl.pallas_call(
        functools.partial(kernel, sp, chips),
        out_shape=[pltpu.VMEM(a.shape, a.dtype) for a in shapes],
        in_specs=[pl.BlockSpec(memory_space=pltpu.MemorySpace.HBM)] * 7,
        out_specs=[pl.BlockSpec(memory_space=pltpu.VMEM)] * 5,
        scratch_shapes=[wide(BF)] * 11
        + [wide(F32)] * 4
        + [pltpu.VMEM((8, width), F32)]
        + [wide(F32)] * 5
        + [state(F32)] * 3
        + [state(BF)] * 4
        + [
            pltpu.VMEM((chips * tokens, 2 * rows), BF),
            pltpu.VMEM((2 * rows, chips * tokens), BF),
            pltpu.VMEM((chips * tokens, width), BF),
            pltpu.VMEM((2 * rows, width), BF),
            pltpu.VMEM((chips * tokens, 2 * rows), BF),
            piece(BF), piece(BF), piece(F32), piece(BF), piece(BF), piece(BF), piece(BF),
        ]
        + [dma(pairs)] * 4
        + [dma(chips)] * 2
        + [dma(chips, pairs)] * 2
        + [pltpu.SemaphoreType.DMA] * 2
        + [dma(chips)] * 2
        + [dma(pairs)] * 6
        + [dma(7)],
        compiler_params=pltpu.CompilerParams(
            collective_id=0, has_side_effects=True, vmem_limit_bytes=VMEM_BYTES - kept),
    )(inputs[0], queries[0], keys[0], values[0], log_decay[0], cotangent[0], value_weight)
    outs = pl.pallas_call(
        write_out,
        out_shape=shapes,
        in_specs=[pl.BlockSpec(memory_space=pl.ANY)] * 5,
        out_specs=[pl.BlockSpec(memory_space=pl.ANY)] * 5,
        scratch_shapes=[dma(5)],
        compiler_params=pltpu.CompilerParams(vmem_limit_bytes=1024 * 1024),
    )(*outs)
    return outs[0][None], outs[1][None], outs[2][None], outs[3][None], outs[4]


def solution(mesh):
    row = P("dp", "sp", None)
    return jax.shard_map(
        functools.partial(per_device, mesh.shape["sp"], mesh.shape["dp"]),
        mesh=mesh,
        in_specs=(row,) * 6 + (P("dp", None),),
        out_specs=(row,) * 4 + (P("dp", None),),
        check_vma=False,
    )
```
